512 devices in a mesh: grp: 2 (over y), fs: 16 (over z), tp: 16 (over x, core).
Axes of the slice: x: 8, y: 2, z: 16, core: 2. Of those that a mesh axis runs over, the one named last changes fastest.
The devices are a block of a 8x16x16 slice.
Arguments:
- tokens: bfloat16 [4096, 2048], P(('grp', 'fs'), 'tp'), parts along dimension 0, may hold values from -40 to 40
- norm_gain: float32 [2048], P('tp'), may hold values from 0.1 to 1.9
- expert_ids: int32 [4096, 8], P(('grp', 'fs')), parts along dimension 0, may hold values from 0 to 63, all different within a row; in each aligned block of 128 rows (0 to 127, 128 to 255, ...) at most 24 rows name the same one
- route_scores: float32 [4096, 8], P(('grp', 'fs')), parts along dimension 0, may hold values from 0.1 to 1
- gate_weight: float32 [64, 512, 2048], P(None, 'fs', 'tp'), may hold values from -0.125 to 0.125
- up_weight: float32 [64, 512, 2048], P(None, 'fs', 'tp'), may hold values from -0.125 to 0.125
- down_weight: float32 [64, 512, 2048], P(None, 'fs', 'tp'), may hold values from -0.25 to 0.25
- shared_gate: float32 [512, 2048], P('fs', 'tp'), may hold values from -0.125 to 0.125
- shared_up: float32 [512, 2048], P('fs', 'tp'), may hold values from -0.125 to 0.125
- shared_down: float32 [512, 2048], P('fs', 'tp'), may hold values from -0.25 to 0.25
Outputs:
- gate_served: bfloat16 [128, 512, 2048], P(('grp', 'fs'), None, 'tp'), parts along dimension 0
- up_served: bfloat16 [128, 512, 2048], P(('grp', 'fs'), None, 'tp'), parts along dimension 0
- down_served: bfloat16 [128, 512, 2048], P(('grp', 'fs'), None, 'tp'), parts along dimension 0
- shared_gate_served: bfloat16 [1024, 2048], P('grp', 'tp'), parts along dimension 0
- shared_up_served: bfloat16 [1024, 2048], P('grp', 'tp'), parts along dimension 0
- shared_down_served: bfloat16 [1024, 2048], P('grp', 'tp'), parts along dimension 0
- layer_output: bfloat16 [4096, 2048], P(('grp', 'fs'), 'tp'), parts along dimension 0
The draws below stay inside these ranges and needn't reach their ends.
There are 2 independent parts, one for each index of `grp`. The reference program is written for one: setup_inputs(seed, part) draws one part's arguments, and reference() takes and returns one part's arrays. A program takes and returns all parts, laid end to end along the dimension named above; an argument that names none is the same for every part. Nothing has to cross between parts.
Inputs may be any that keep to these rules, and one draw needn't show every extreme that they name: `expert_ids`: each row names 8 different experts. Among the rows of one index of fs no expert is named more than 24 times; in every draw some expert reaches 24 on some index of fs.
All inputs are finite; a program needn't handle non-finite values.
Results may differ from the reference program's by a relative error of at most 0.03.
Values may be sent and summed in bfloat16 or wider, within the bound.
A program may use at most 64 MiB of HBM per device.

```python
import math
import jax
import jax.numpy as jnp
import numpy as np
from jax import lax

D = 2048
FF = 512
EXPERTS = 64
TOP_K = 8
TOK_DEV = 128
CAPACITY = 24
TOKENS = 2048
N_FS = 16
N_TP = 16


def draw_tokens(key, part):
    draw_key = jax.random.fold_in(key, 0)
    column = 3.0 ** (jnp.arange(D, dtype=jnp.float32) / (D - 1))
    values = jnp.clip(jax.random.normal(draw_key, (TOKENS, D), jnp.float32), -8.0, 8.0)
    return (values * column[None, :]).astype(jnp.bfloat16)


def levels(rng, extent, cuts, smallest, top_value):
    def one(dim, shards_of):
        heights = jax.random.uniform(jax.random.fold_in(jax.random.fold_in(rng, 6), dim), (shards_of,), jnp.float32, smallest / len(cuts), top_value / len(cuts))
        return jnp.repeat(jnp.exp(heights), extent[dim] // shards_of).reshape((-1,) + (1,) * (len(extent) - dim - 1))

    loudness = one(*cuts[0])
    for cut in cuts[1:]:
        loudness = loudness * one(*cut)
    return loudness


def assign_block(stream_key, own, number, rows, number_of, top, most, lean):
    sequence = jax.random.permutation(stream_key, number_of)
    heavy_load, common = load_shares(number_of, rows * top, most, lean, True), load_shares(number_of, rows * top, most, lean, False)
    places = jnp.arange(number_of)

    def named(lengths, rotation):
        used = int((lengths > 0).sum())
        fixed = max(1, used // 4)
        passed = fixed + (places - fixed + rotation * (used - fixed)) % max(1, number_of - fixed)
        return jnp.zeros((number_of,), jnp.int32).at[sequence[jnp.where(places < fixed, places, passed)]].set(jnp.asarray(lengths, jnp.int32))

    lengths = jnp.where(number % 4 == 0, named(heavy_load, number // 4), named(common, number - number // 4 - 1))
    mixed = jax.random.permutation(jax.random.fold_in(own, 3), number_of)
    source_of, receiver = mixed[0:number_of // 2 * 2:2], mixed[1:number_of // 2 * 2:2]
    margin = jnp.minimum(lengths[source_of] - 1, most - lengths[receiver]) // 2
    margin = jnp.where((source_of == sequence[0]) | (receiver == sequence[0]) | (lengths[receiver] == 0), 0, jnp.maximum(margin, 0))
    passed = jax.random.randint(jax.random.fold_in(own, 4), (number_of // 2,), 0, 1 << 20) % (margin + 1)
    lengths = lengths.at[source_of].add(-passed).at[receiver].add(passed)
    members = jnp.searchsorted(jnp.cumsum(lengths), jnp.arange(rows * top), side="right").astype(jnp.int32)
    table = members.reshape(top, rows).T
    table = table[jax.random.permutation(jax.random.fold_in(own, 1), rows)]
    rotation = jax.random.randint(jax.random.fold_in(own, 2), (rows, 1), 0, top)
    return jnp.take_along_axis(table, (jnp.arange(top)[None, :] + rotation) % top, axis=1)


def load_shares(amount, total, most, lean, full):
    loads = [(1 << 20) // math.isqrt(standing ** lean) + 1 for standing in range(1, amount + 1)]
    largest = most if full else min(most, max(-(-total // amount), total * loads[0] // sum(loads)))
    least = 1 if total - largest >= amount - 1 else 0
    counts, spare = [largest] + [least] * (amount - 1), total - largest - least * (amount - 1)
    while spare > 0:
        movable = [i for i in range(1, amount) if counts[i] < largest] or [i for i in range(1, amount) if counts[i] < most]
        mass, remaining = sum([loads[i] for i in movable]), spare
        for i in movable:
            addition = min(most - counts[i], max(1, remaining * loads[i] // mass), spare)
            counts[i] = counts[i] + addition
            spare = spare - addition
    return np.array(counts)


def centred(key, shape, deviation, limit, cuts=(), kind=jnp.bfloat16):
    level = levels(key, shape, cuts, -0.22, 0.18) if cuts else 1.0
    array = jax.random.normal(key, shape, jnp.float32) * deviation * level
    return jnp.minimum(jnp.maximum(array, -limit), limit).astype(kind)


def setup_inputs(seed: int = 0, part: int = 0) -> dict:
    key_of = jax.random.split(jax.random.key(seed), 11)
    own_keys = jax.random.split(jax.random.fold_in(key_of[10], part), 11)
    tokens = draw_tokens(jax.random.fold_in(jax.random.fold_in(key_of[10], part), 71), part)
    norm_gain = jnp.clip(1.0 + 0.18 * jax.random.normal(key_of[1], (D,), jnp.float32), 0.1, 1.9)
    expert_ids_keys = jax.random.split(jax.random.fold_in(own_keys[2], 1), TOKENS // TOK_DEV)
    expert_ids_turns = jax.random.permutation(jax.random.fold_in(own_keys[2], 3), TOKENS // TOK_DEV)
    expert_ids = jax.vmap(lambda own, number: assign_block(jax.random.fold_in(own_keys[2], 2), own, number, TOK_DEV, EXPERTS, TOP_K, CAPACITY, 2))(expert_ids_keys, expert_ids_turns).reshape((TOKENS, TOP_K))
    route_scores = jnp.clip(jnp.exp(math.log(1.0) - 2.3025851 * jax.random.uniform(own_keys[3], (TOKENS, TOP_K), jnp.float32) ** levels(own_keys[3], (TOKENS, TOP_K), ((0, 16),), -0.2, 0.2)), 0.1, 1.0)
    gate_weight = centred(key_of[4], (EXPERTS, FF, D), D ** -0.5, 0.125, ((1, 16), (2, 16)), jnp.float32)
    up_weight = centred(key_of[5], (EXPERTS, FF, D), D ** -0.5, 0.125, ((1, 16), (2, 16)), jnp.float32)
    down_weight = centred(key_of[6], (EXPERTS, FF, D), FF ** -0.5, 0.25, ((1, 16), (2, 16)), jnp.float32)
    shared_gate = centred(key_of[7], (FF, D), D ** -0.5, 0.125, ((0, 16), (1, 16)), jnp.float32)
    shared_up = centred(key_of[8], (FF, D), D ** -0.5, 0.125, ((0, 16), (1, 16)), jnp.float32)
    shared_down = centred(key_of[9], (FF, D), FF ** -0.5, 0.25, ((0, 16), (1, 16)), jnp.float32)
    return dict(tokens=tokens, norm_gain=norm_gain, expert_ids=expert_ids, route_scores=route_scores, gate_weight=gate_weight, up_weight=up_weight, down_weight=down_weight, shared_gate=shared_gate, shared_up=shared_up, shared_down=shared_down)


norm_eps = 1e-05
routed_scale = 2.5

def normalize(tokens):
    tok_float = tokens.astype(jnp.float32)
    full_width = tok_float.shape[1]
    row_mean = lax.optimization_barrier(jnp.sum(tok_float, axis=1)) / full_width
    row_var = lax.optimization_barrier(jnp.sum(tok_float * tok_float, axis=1)) / full_width - row_mean * row_mean
    return ((tok_float - row_mean[:, None]) * lax.rsqrt(row_var + norm_eps)[:, None]).astype(jnp.bfloat16)

def blocked_hidden(rows_in, paired):
    count_rows = rows_in.shape[0]
    split_rows = rows_in.astype(jnp.float32).reshape(count_rows, N_TP, -1)
    split_pair = paired.astype(jnp.float32).reshape(paired.shape[0], N_TP, -1)
    partial_value = jnp.einsum('ntd,ftd->tnf', split_rows, split_pair).astype(jnp.bfloat16)
    summed = lax.optimization_barrier(jnp.sum(partial_value.astype(jnp.float32), axis=0))
    return (jax.nn.silu(summed[:, :FF]) * summed[:, FF:]).astype(jnp.bfloat16)

def reference(tokens, norm_gain, expert_ids, route_scores, gate_weight, up_weight, down_weight, shared_gate, shared_up, shared_down):
    normed = normalize(tokens)
    gate_new = (gate_weight * norm_gain[None, None, :]).astype(jnp.bfloat16)
    up_new = (up_weight * norm_gain[None, None, :]).astype(jnp.bfloat16)
    down_new = down_weight.astype(jnp.bfloat16)
    gate_shared = (shared_gate * norm_gain[None, :]).astype(jnp.bfloat16)
    up_shared = (shared_up * norm_gain[None, :]).astype(jnp.bfloat16)
    down_shared = shared_down.astype(jnp.bfloat16)
    route_weight = route_scores / lax.optimization_barrier(jnp.sum(route_scores, axis=1, keepdims=True)) * routed_scale
    flat_ids = expert_ids.reshape(-1)
    assignments = flat_ids.shape[0]
    flat_tokens = jnp.concatenate([jnp.arange(assignments, dtype=jnp.int32) // TOP_K, jnp.full((1,), TOKENS, jnp.int32)])
    flat_weight = jnp.concatenate([route_weight.reshape(-1), jnp.zeros((1,), jnp.float32)])
    padded = jnp.concatenate([normed, jnp.zeros((1, D), jnp.bfloat16)], axis=0)

    def one_expert(running, expert):
        chosen = jnp.nonzero(flat_ids == expert, size=N_FS * CAPACITY, fill_value=assignments)[0].astype(jnp.int32)
        token_rows = flat_tokens[chosen]
        paired = jnp.concatenate([gate_new[expert], up_new[expert]], axis=0)
        hidden = blocked_hidden(padded[token_rows], paired)
        result = jnp.dot(hidden, down_new[expert], preferred_element_type=jnp.float32).astype(jnp.bfloat16)
        return (running.at[token_rows].add(result.astype(jnp.float32) * flat_weight[chosen][:, None]), None)
    routed, _ = lax.scan(one_expert, jnp.zeros((TOKENS + 1, D), jnp.float32), jnp.arange(EXPERTS, dtype=jnp.int32))
    shared_hidden = blocked_hidden(normed, jnp.concatenate([gate_shared, up_shared], axis=0))
    shared_out = jnp.dot(shared_hidden, down_shared, preferred_element_type=jnp.float32)
    layer_out = (shared_out + routed[:TOKENS]).astype(jnp.bfloat16)
    return (gate_new, up_new, down_new, gate_shared, up_shared, down_shared, layer_out)
```

```python
import functools

import jax
import jax.numpy as jnp
from jax import lax
from jax.experimental import pallas as pl
from jax.experimental.pallas import tpu as pltpu
from jax.sharding import PartitionSpec as P

CAPACITY = 24
NORM_EPS = 1e-05
ROUTED_SCALE = 2.5
MESH = pl.DeviceIdType.MESH
F32 = jnp.float32
BF16 = jnp.bfloat16


def nt_dot(a, b):
    return lax.dot_general(a, b, (((1,), (1,)), ((), ())), preferred_element_type=F32)


def nn_dot(a, b):
    return jnp.dot(a, b, preferred_element_type=F32)


def layer_kernel(
    nz, nt, full_width,
    tok_ref, gain_ref, ids_ref, score_ref, gate_ref, up_ref, down_ref, sg_ref, su_ref, sd_ref,
    o1, o2, osh, out_ref,
    w1, w2, ws, stat, xs, xr, own, pdo, pdr, q, rr, h, rb, rt, sel_hi, sel_lo, nrm_ref,
    st_s, st_r, tk_s, tk_r, w1_s, w1_r, f1_s, f1_r, w2_s, w2_r, f2_s, f2_r, sh_s, sh_r, fs_s, fs_r,
    dd_s, dd_r, rs_s, rs_r, ag_s, ag_r, fw_s, fw_r, re_s, re_r,
):
    z = lax.axis_index("fs")
    t = lax.axis_index("tp")
    g = lax.axis_index("grp")
    y = lax.rem(g, 2)
    mate = g + 1 - 2 * y
    core = lax.rem(t, 2)
    x = t // 2
    nx = nt // 2
    twin = t + 1 - 2 * core

    experts, ff_here, width = gate_ref.shape
    eh = experts // nz
    ff = ff_here * nz
    half = ff // 2
    toks = tok_ref.shape[0]
    cap_rows = nz * CAPACITY
    seg = cap_rows // nx
    sseg = toks // nx
    units = eh + 1

    def unit_rows(u):
        return (u * seg, seg) if u < eh else (eh * seg, sseg)

    def rcopy(src, dst, ss, rs, **where):
        return pltpu.make_async_remote_copy(
            src_ref=src, dst_ref=dst, send_sem=ss, recv_sem=rs, device_id=where, device_id_type=MESH
        )

    def each(n, me, body):
        def step(k, carry):
            body(lax.rem(me + k, n))
            return carry

        lax.fori_loop(1, n, step, 0)

    barrier = pltpu.get_barrier_semaphore()
    each(nz, z, lambda d: pl.semaphore_signal(barrier, inc=1, device_id={"fs": d}, device_id_type=MESH))
    each(nt, t, lambda d: pl.semaphore_signal(barrier, inc=1, device_id={"tp": d}, device_id_type=MESH))
    pl.semaphore_signal(barrier, inc=1, device_id={"grp": mate}, device_id_type=MESH)

    gain = gain_ref[...]
    w1[0] = (gate_ref[...] * gain[None]).astype(BF16)
    w1[1] = (up_ref[...] * gain[None]).astype(BF16)
    w2[...] = down_ref[...].astype(BF16)
    hr = ff_here // 2
    ws[0] = (sg_ref[...] * gain).astype(BF16).reshape(2, hr, width)
    ws[1] = (su_ref[...] * gain).astype(BF16).reshape(2, hr, width)
    ws[2] = sd_ref[...].astype(BF16).reshape(2, hr, width)
    rows_z = pl.ds(pl.multiple_of(z * ff_here, ff_here), ff_here)
    o1[y, :, rows_z, :] = w1[y, pl.ds(eh * z, eh)]
    o2[pl.ds(2 * y, 2), rows_z, :] = w2[pl.ds(eh * z + 2 * y, 2)]
    osh[:, z, y] = ws[:, y]

    tok_t = tok_ref[...].astype(F32).T
    stat[t] = jnp.concatenate(
        [
            jnp.sum(tok_t, axis=0, keepdims=True),
            jnp.sum(tok_t * tok_t, axis=0, keepdims=True),
            jnp.zeros((6, toks), F32),
        ],
        axis=0,
    )

    pl.semaphore_wait(barrier, nz + nt - 1)

    def stat_copy(src, dst):
        return rcopy(stat.at[src], stat.at[src], st_s.at[dst], st_r.at[src], tp=dst)

    each(nt, t, lambda d: stat_copy(t, d).start())

    def w1_copy(e, src, dst):
        return rcopy(
            w1.at[y, eh * dst + e],
            o1.at[y, e, pl.ds(pl.multiple_of(src * ff_here, ff_here), ff_here), :],
            w1_s.at[e, dst], w1_r.at[e, src], fs=dst,
        )

    def w2_copy(src, dst):
        return rcopy(
            w2.at[pl.ds(eh * dst + 2 * y, 2)],
            o2.at[pl.ds(2 * y, 2), pl.ds(pl.multiple_of(src * ff_here, ff_here), ff_here), :],
            w2_s.at[dst], w2_r.at[src], fs=dst,
        )

    def sh_copy(src, dst):
        return rcopy(ws.at[:, y], osh.at[:, src, y], sh_s.at[dst], sh_r.at[src], fs=dst)

    def tk_copy(src, dst):
        return rcopy(xs.at[dst], xr.at[src], tk_s.at[dst], tk_r.at[src], fs=dst)

    each(nz, z, lambda d: w1_copy(0, z, d).start())

    ids = ids_ref[...]
    scores = score_ref[...]
    weight = scores / jnp.sum(scores, axis=1, keepdims=True) * ROUTED_SCALE
    lane = lax.broadcasted_iota(jnp.int32, (toks, 128), 1)
    chosen = jnp.zeros((toks, 128), F32)
    spread = jnp.zeros((toks, 128), F32)
    for k in range(ids.shape[1]):
        hit = ids[:, k : k + 1] == lane
        chosen = chosen + jnp.where(hit, 1.0, 0.0)
        spread = spread + jnp.where(hit, weight[:, k : k + 1], 0.0)
    below = lax.broadcasted_iota(jnp.int32, (toks, toks), 1) < lax.broadcasted_iota(
        jnp.int32, (toks, toks), 0
    )
    rank = nn_dot(jnp.where(below, 1.0, 0.0).astype(BF16), chosen.astype(BF16))
    rank = jnp.where(chosen > 0.5, rank, -1.0)
    rank_t = rank.T[:experts]
    slot = lax.broadcasted_iota(jnp.int32, (experts, CAPACITY, toks), 1).astype(F32)
    pick = jnp.where(rank_t[:, None, :] == slot, 1.0, 0.0).reshape(experts * CAPACITY, toks)
    pick = pick.astype(BF16)

    each(nt, t, lambda d: stat_copy(d, t).wait_recv())
    total = jnp.sum(stat[...], axis=0)
    mean = total[0:1] / full_width
    var = total[1:2] / full_width - mean * mean
    nrm = ((tok_t - mean) * lax.rsqrt(var + NORM_EPS)).T.astype(BF16)
    nrm_ref[...] = nrm
    xs[...] = nn_dot(pick, nrm).astype(BF16).reshape(nz, eh * CAPACITY, width)
    each(nz, z, lambda d: tk_copy(z, d).start())
    for e in range(1, eh):
        each(nz, z, lambda d: w1_copy(e, z, d).start())
    each(nz, z, lambda d: sh_copy(z, d).start())
    each(nz, z, lambda d: w2_copy(z, d).start())

    xr[z] = xs[z]
    row = lax.broadcasted_iota(jnp.int32, (128, experts * CAPACITY), 0) * CAPACITY
    col = lax.broadcasted_iota(jnp.int32, (128, experts * CAPACITY), 1)
    wide = jnp.where((col >= row) & (col < row + CAPACITY), 1.0, 0.0).astype(BF16)
    colf = col[:toks].astype(F32)
    col_slot = colf - jnp.floor((colf + 0.5) * (1.0 / CAPACITY)) * CAPACITY
    mine = nn_dot(rank.astype(BF16), wide) == col_slot
    hi = spread.astype(BF16)
    lo = (spread - hi.astype(F32)).astype(BF16)
    sel_hi[...] = jnp.where(mine, nn_dot(hi, wide), 0.0).astype(BF16)
    sel_lo[...] = jnp.where(mine, nn_dot(lo, wide), 0.0).astype(BF16)

    def f1_copy(e, side):
        return rcopy(o1.at[side, e], o1.at[side, e], f1_s.at[e], f1_r.at[e], grp=mate)

    def f2_copy(side):
        part = o2.at[pl.ds(2 * side, 2)]
        return rcopy(part, part, f2_s, f2_r, grp=mate)

    def fs_copy(side):
        return rcopy(osh.at[:, :, side], osh.at[:, :, side], fs_s, fs_r, grp=mate)

    def dd_copy(u):
        r0, n = unit_rows(u)
        rows = pl.ds(nx * r0, nx * n)
        return rcopy(pdo.at[rows], pdr.at[rows], dd_s.at[u], dd_r.at[u], tp=twin)

    def rs_copy(u, src, dst):
        r0, n = unit_rows(u)
        rows = pl.ds(r0, n)
        return rcopy(q.at[dst, rows], rr.at[src, rows], rs_s.at[u, dst], rs_r.at[u, src], tp=2 * dst + core)

    def ag_copy(u, src, dst):
        r0, n = unit_rows(u)
        part = h.at[core, src, pl.ds(r0, n)]
        return rcopy(part, part, ag_s.at[u, dst], ag_r.at[u, src], tp=2 * dst + core)

    def fw_copy(u, src, side):
        r0, n = unit_rows(u)
        part = h.at[side, src, pl.ds(r0, n)]
        return rcopy(part, part, fw_s.at[u, src], fw_r.at[u, src], tp=twin)

    def re_copy(p, src, dst):
        rows = pl.ds(2 * CAPACITY * p, 2 * CAPACITY)
        return rcopy(rb.at[dst, rows], rt.at[src, rows], re_s.at[p, dst], re_r.at[p, src], fs=dst)

    def paired(u, part):
        cols = pl.ds(pl.multiple_of(part * half, half), half)
        if u < eh:
            return jnp.concatenate([o1[0, u, cols, :], o1[1, u, cols, :]], axis=0)
        zs = pl.ds(part * (nz // 2), nz // 2)
        return jnp.concatenate(
            [osh[0, zs].reshape(half, width), osh[1, zs].reshape(half, width)], axis=0
        )

    def first_matmul(u):
        r0, n = unit_rows(u)
        if u < eh:
            arrived = xr[...].astype(F32)[:, u * CAPACITY : (u + 1) * CAPACITY, :]
            rows_in = arrived.reshape(cap_rows, width).astype(BF16)
        else:
            rows_in = nrm_ref[...]
        pdo[nx * r0 : nx * (r0 + n), :] = nt_dot(rows_in, paired(u, 1 - core)).astype(BF16)
        dd_copy(u).start()
        own[nx * r0 : nx * (r0 + n), :] = nt_dot(rows_in, paired(u, core))

    def chip_sum(u):
        r0, n = unit_rows(u)
        rows = slice(nx * r0, nx * (r0 + n))
        dd_copy(u).wait_recv()
        both = own[rows, :] + pdr[rows, :].astype(F32)
        q[:, r0 : r0 + n, :] = both.astype(BF16).reshape(nx, n, 2 * half)
        each(nx, x, lambda d: rs_copy(u, x, d).start())
        rr[x, r0 : r0 + n, :] = q[x, r0 : r0 + n, :]

    def activate(u):
        r0, n = unit_rows(u)
        each(nx, x, lambda d: rs_copy(u, d, x).wait_recv())
        pre = jnp.sum(rr[:, r0 : r0 + n, :].astype(F32), axis=0)
        h[core, x, r0 : r0 + n, :] = (jax.nn.silu(pre[:, :half]) * pre[:, half:]).astype(BF16)
        each(nx, x, lambda d: ag_copy(u, x, d).start())
        fw_copy(u, x, core).start()

    def pass_on(u):
        def one(d):
            ag_copy(u, d, x).wait_recv()
            fw_copy(u, d, core).start()

        each(nx, x, one)

    def hidden_part(u, part):
        r0, n = unit_rows(u)
        return h[part, :, r0 : r0 + n, :].reshape(nx * n, half)

    def all_hidden(u):
        def one(k, carry):
            fw_copy(u, k, 1 - core).wait_recv()
            return carry

        lax.fori_loop(0, nx, one, 0)

    def arrivals(e):
        each(nz, z, lambda d: w1_copy(e, d, z).wait_recv())
        f1_copy(e, y).start()

    arrivals(0)
    each(nz, z, lambda d: tk_copy(d, z).wait_recv())
    for e in range(eh):
        f1_copy(e, 1 - y).wait_recv()
        first_matmul(e)
        if e + 1 < eh:
            arrivals(e + 1)
        chip_sum(e)
    each(nz, z, lambda d: sh_copy(d, z).wait_recv())
    fs_copy(y).start()
    each(nz, z, lambda d: w2_copy(d, z).wait_recv())
    f2_copy(y).start()
    fs_copy(1 - y).wait_recv()
    first_matmul(eh)
    chip_sum(eh)
    for u in range(units):
        activate(u)
        if u > 0:
            pass_on(u - 1)
    pass_on(units - 1)
    f2_copy(1 - y).wait_recv()
    for p in range(eh // 2):
        both = []
        for u in (2 * p, 2 * p + 1):
            all_hidden(u)
            res = nn_dot(hidden_part(u, 0), o2[u, :half, :]) + nn_dot(hidden_part(u, 1), o2[u, half:, :])
            both.append(res.reshape(nz, CAPACITY, width))
        rb[:, 2 * CAPACITY * p : 2 * CAPACITY * (p + 1), :] = jnp.concatenate(both, axis=1).astype(BF16)
        each(nz, z, lambda d: re_copy(p, z, d).start())
    rt[z] = rb[z]
    all_hidden(eh)
    down = osh[2].reshape(ff, width)
    shared = nn_dot(hidden_part(eh, 0), down[:half]) + nn_dot(hidden_part(eh, 1), down[half:])
    for p in range(eh // 2):
        each(nz, z, lambda d: re_copy(p, d, z).wait_recv())
    back = rt[...].reshape(experts * CAPACITY, width)
    out_ref[...] = (nn_dot(sel_hi[...], back) + nn_dot(sel_lo[...], back) + shared).astype(BF16)

    each(nt, t, lambda d: stat_copy(t, d).wait_send())
    each(nz, z, lambda d: tk_copy(z, d).wait_send())
    for e in range(eh):
        each(nz, z, lambda d: w1_copy(e, z, d).wait_send())
        f1_copy(e, y).wait_send()
    each(nz, z, lambda d: w2_copy(z, d).wait_send())
    f2_copy(y).wait_send()
    each(nz, z, lambda d: sh_copy(z, d).wait_send())
    fs_copy(y).wait_send()
    for u in range(units):
        dd_copy(u).wait_send()
        each(nx, x, lambda d: rs_copy(u, x, d).wait_send())
        each(nx, x, lambda d: ag_copy(u, x, d).wait_send())
        fw_copy(u, x, core).wait_send()
        each(nx, x, lambda d: fw_copy(u, d, core).wait_send())
    for p in range(eh // 2):
        each(nz, z, lambda d: re_copy(p, z, d).wait_send())


def on_device(nz, nt, tokens, norm_gain, expert_ids, route_scores, gate, up, down, sg, su, sd):
    experts, ff_here, width = gate.shape
    eh = experts // nz
    ff = ff_here * nz
    half = ff // 2
    toks = tokens.shape[0]
    nx = nt // 2
    rows = eh * nz * CAPACITY + toks
    disp = (nz, eh * CAPACITY, width)
    units = eh + 1
    vmem = pl.BlockSpec(memory_space=pltpu.VMEM)
    dma = pltpu.SemaphoreType.DMA
    pairs = eh // 2
    sems = []
    for shape in (
        (nt,), (nz,), (eh, nz), (eh,), (nz,), (), (nz,), (), (units,), (units, nx), (units, nx), (units, nx), (pairs, nz),
    ):
        sems += [dma(shape), dma(shape)]
    o1, o2, osh, out = pl.pallas_call(
        functools.partial(layer_kernel, nz, nt, width * nt),
        out_shape=(
            jax.ShapeDtypeStruct((2, eh, ff, width), BF16),
            jax.ShapeDtypeStruct((eh, ff, width), BF16),
            jax.ShapeDtypeStruct((3, nz, 2, ff_here // 2, width), BF16),
            jax.ShapeDtypeStruct((toks, width), BF16),
        ),
        in_specs=[vmem] * 10,
        out_specs=(vmem,) * 4,
        scratch_shapes=[
            pltpu.VMEM((2, experts, ff_here, width), BF16),
            pltpu.VMEM((experts, ff_here, width), BF16),
            pltpu.VMEM((3, 2, ff_here // 2, width), BF16),
            pltpu.VMEM((nt, 8, toks), F32),
            pltpu.VMEM(disp, BF16),
            pltpu.VMEM(disp, BF16),
            pltpu.VMEM((rows, 2 * half), F32),
            pltpu.VMEM((rows, 2 * half), BF16),
            pltpu.VMEM((rows, 2 * half), BF16),
            pltpu.VMEM((nx, rows // nx, 2 * half), BF16),
            pltpu.VMEM((nx, rows // nx, 2 * half), BF16),
            pltpu.VMEM((2, nx, rows // nx, half), BF16),
            pltpu.VMEM(disp, BF16),
            pltpu.VMEM(disp, BF16),
            pltpu.VMEM((toks, experts * CAPACITY), BF16),
            pltpu.VMEM((toks, experts * CAPACITY), BF16),
            pltpu.VMEM((toks, width), BF16),
            *sems,
        ],
        compiler_params=pltpu.CompilerParams(
            collective_id=0, has_side_effects=True, vmem_limit_bytes=56 * 1024 * 1024
        ),
        name="layer",
    )(tokens, norm_gain.reshape(1, width), expert_ids, route_scores, gate, up, down, sg, su, sd)
    osh = osh.reshape(3, ff, width)
    return o1[0], o1[1], o2, osh[0], osh[1], osh[2], out


def solution(mesh):
    return jax.shard_map(
        functools.partial(on_device, mesh.shape["fs"], mesh.shape["tp"]),
        mesh=mesh,
        in_specs=(
            P(("grp", "fs"), "tp"),
            P("tp"),
            P(("grp", "fs"), None),
            P(("grp", "fs"), None),
            P(None, "fs", "tp"),
            P(None, "fs", "tp"),
            P(None, "fs", "tp"),
            P("fs", "tp"),
            P("fs", "tp"),
            P("fs", "tp"),
        ),
        out_specs=(
            P(("grp", "fs"), None, "tp"),
            P(("grp", "fs"), None, "tp"),
            P(("grp", "fs"), None, "tp"),
            P("grp", "tp"),
            P("grp", "tp"),
            P("grp", "tp"),
            P(("grp", "fs"), "tp"),
        ),
        check_vma=False,
    )
```

```python
import functools

import jax
import jax.numpy as jnp
from jax import lax
from jax.experimental import pallas as pl
from jax.experimental.pallas import tpu as pltpu
from jax.sharding import PartitionSpec as P

CAPACITY = 24
NORM_EPS = 1e-05
ROUTED_SCALE = 2.5
MESH = pl.DeviceIdType.MESH
F32 = jnp.float32
BF16 = jnp.bfloat16


def nt_dot(a, b):
    return lax.dot_general(a, b, (((1,), (1,)), ((), ())), preferred_element_type=F32)


def nn_dot(a, b):
    return jnp.dot(a, b, preferred_element_type=F32)


def layer_kernel(
    nz, nt, full_width,
    tok_ref, gain_ref, ids_ref, score_ref, gate_hbm, up_hbm, down_hbm, sg_ref, su_ref, sd_ref,
    og_hbm, ou_hbm, od_hbm, osg_hbm, osu_hbm, osd_hbm, out_ref,
    gate_ref, up_ref, down_ref, og, ou, o2, osg, osu, osd, in_sem, out_sem,
    osh, w1, w2, ws, stat, xs, xr, own, pdo, pdr, q, rr, h, rb, rt, sel_hi, sel_lo, nrm_ref,
    st_s, st_r, tk_s, tk_r, w1_s, w1_r, f1_s, f1_r, w2_s, w2_r, f2_s, f2_r, sh_s, sh_r, fs_s, fs_r,
    dd_s, dd_r, rs_s, rs_r, ag_s, ag_r, fw_s, fw_r, re_s, re_r,
):
    z = lax.axis_index("fs")
    t = lax.axis_index("tp")
    g = lax.axis_index("grp")
    y = lax.rem(g, 2)
    mate = g + 1 - 2 * y
    core = lax.rem(t, 2)
    x = t // 2
    nx = nt // 2
    twin = t + 1 - 2 * core
    ahead = 1 - 2 * core
    n_long = nx // 2
    n_short = nx - 1 - n_long
    o1 = (og, ou)

    experts, ff_here, width = gate_hbm.shape
    eh = experts // nz
    ff = ff_here * nz
    half = ff // 2
    toks = tok_ref.shape[0]
    cap_rows = nz * CAPACITY
    seg = cap_rows // nx
    sseg = toks // nx
    units = eh + 1

    def unit_rows(u):
        return (u * seg, seg) if u < eh else (eh * seg, sseg)

    def rcopy(src, dst, ss, rs, **where):
        return pltpu.make_async_remote_copy(
            src_ref=src, dst_ref=dst, send_sem=ss, recv_sem=rs, device_id=where, device_id_type=MESH
        )

    def each(n, me, body):
        def step(k, carry):
            body(lax.rem(me + k, n))
            return carry

        lax.fori_loop(1, n, step, 0)

    barrier = pltpu.get_barrier_semaphore()
    each(nz, z, lambda d: pl.semaphore_signal(barrier, inc=1, device_id={"fs": d}, device_id_type=MESH))
    each(nt, t, lambda d: pl.semaphore_signal(barrier, inc=1, device_id={"tp": d}, device_id_type=MESH))
    pl.semaphore_signal(barrier, inc=1, device_id={"grp": mate}, device_id_type=MESH)

    loads = [
        pltpu.make_async_copy(src, dst, in_sem.at[i])
        for i, (src, dst) in enumerate(((gate_hbm, gate_ref), (up_hbm, up_ref), (down_hbm, down_ref)))
    ]
    for load in loads:
        load.start()
    stores = [
        pltpu.make_async_copy(src, dst, out_sem.at[i])
        for i, (src, dst) in enumerate(
            ((og, og_hbm), (ou, ou_hbm), (o2, od_hbm), (osg, osg_hbm), (osu, osu_hbm), (osd, osd_hbm))
        )
    ]
    gain = gain_ref[...]
    hr = ff_here // 2
    ws[0] = (sg_ref[...] * gain).astype(BF16).reshape(2, hr, width)
    ws[1] = (su_ref[...] * gain).astype(BF16).reshape(2, hr, width)
    ws[2] = sd_ref[...].astype(BF16).reshape(2, hr, width)
    loads[0].wait()
    w1[0] = (gate_ref[...] * gain[None]).astype(BF16)
    loads[1].wait()
    w1[1] = (up_ref[...] * gain[None]).astype(BF16)
    loads[2].wait()
    w2[...] = down_ref[...].astype(BF16)
    rows_z = pl.ds(pl.multiple_of(z * ff_here, ff_here), ff_here)

    def on_side(body):
        for side in (0, 1):
            pl.when(y == side)(functools.partial(body, side))

    def keep_own(side):
        o1[side][:, rows_z, :] = w1[side, pl.ds(eh * z, eh)]

    on_side(keep_own)
    o2[pl.ds((eh // 2) * y, eh // 2), rows_z, :] = w2[pl.ds(eh * z + (eh // 2) * y, eh // 2)]
    osh[:, z, y] = ws[:, y]

    tok_t = tok_ref[...].astype(F32).T
    stat[t] = jnp.concatenate(
        [
            jnp.sum(tok_t, axis=0, keepdims=True),
            jnp.sum(tok_t * tok_t, axis=0, keepdims=True),
            jnp.zeros((6, toks), F32),
        ],
        axis=0,
    )

    pl.semaphore_wait(barrier, nz + nt - 1)

    def stat_copy(src, dst):
        return rcopy(stat.at[src], stat.at[src], st_s.at[dst], st_r.at[src], tp=dst)

    each(nt, t, lambda d: stat_copy(t, d).start())

    def w1_copy(side, e, src, dst):
        return rcopy(
            w1.at[side, eh * dst + e],
            o1[side].at[e, pl.ds(pl.multiple_of(src * ff_here, ff_here), ff_here), :],
            w1_s.at[e, dst], w1_r.at[e, src], fs=dst,
        )

    def w2_copy(j, src, dst):
        return rcopy(
            w2.at[eh * dst + (eh // 2) * y + j],
            o2.at[(eh // 2) * y + j, pl.ds(pl.multiple_of(src * ff_here, ff_here), ff_here), :],
            w2_s.at[j, dst], w2_r.at[j, src], fs=dst,
        )

    def sh_copy(src, dst):
        return rcopy(ws.at[:, y], osh.at[:, src, y], sh_s.at[dst], sh_r.at[src], fs=dst)

    def tk_copy(src, dst):
        return rcopy(xs.at[dst], xr.at[src], tk_s.at[dst], tk_r.at[src], fs=dst)

    def send_w1(first, last):
        def one(side):
            for e in range(first, last):
                each(nz, z, lambda d: w1_copy(side, e, z, d).start())

        on_side(one)

    send_w1(0, 1)

    ids = ids_ref[...]
    scores = score_ref[...]
    weight = scores / jnp.sum(scores, axis=0, keepdims=True) * ROUTED_SCALE
    expert = lax.broadcasted_iota(jnp.int32, (experts, toks), 0)
    chosen = jnp.zeros((experts, toks), F32)
    spread = jnp.zeros((experts, toks), F32)
    for k in range(ids.shape[0]):
        hit = ids[k : k + 1] == expert
        chosen = chosen + jnp.where(hit, 1.0, 0.0)
        spread = spread + jnp.where(hit, weight[k : k + 1], 0.0)
    above = lax.broadcasted_iota(jnp.int32, (toks, toks), 0) < lax.broadcasted_iota(
        jnp.int32, (toks, toks), 1
    )
    rank_t = nn_dot(chosen.astype(BF16), jnp.where(above, 1.0, 0.0).astype(BF16))
    rank_t = jnp.where(chosen > 0.5, rank_t, -1.0)
    slot = lax.broadcasted_iota(jnp.int32, (experts, CAPACITY, toks), 1).astype(F32)
    pick = jnp.where(rank_t[:, None, :] == slot, 1.0, 0.0).reshape(experts * CAPACITY, toks)
    pick = pick.astype(BF16)

    each(nt, t, lambda d: stat_copy(d, t).wait_recv())
    total = jnp.sum(stat[...], axis=0)
    mean = total[0:1] / full_width
    var = total[1:2] / full_width - mean * mean
    nrm = ((tok_t - mean) * lax.rsqrt(var + NORM_EPS)).T.astype(BF16)
    nrm_ref[...] = nrm
    xs[...] = nn_dot(pick, nrm).astype(BF16).reshape(nz, eh * CAPACITY, width)
    each(nz, z, lambda d: tk_copy(z, d).start())
    send_w1(1, eh)
    each(nz, z, lambda d: sh_copy(z, d).start())
    for j in range(eh // 2):
        each(nz, z, lambda d: w2_copy(j, z, d).start())

    xr[z] = xs[z]
    rank = jnp.concatenate([rank_t, jnp.full((toks - experts, toks), -1.0, F32)], axis=0).T
    spread = jnp.concatenate([spread, jnp.zeros((toks - experts, toks), F32)], axis=0).T
    row = lax.broadcasted_iota(jnp.int32, (toks, experts * CAPACITY), 0) * CAPACITY
    col = lax.broadcasted_iota(jnp.int32, (toks, experts * CAPACITY), 1)
    wide = jnp.where((col >= row) & (col < row + CAPACITY), 1.0, 0.0).astype(BF16)
    colf = col.astype(F32)
    col_slot = colf - jnp.floor((colf + 0.5) * (1.0 / CAPACITY)) * CAPACITY
    mine = nn_dot(rank.astype(BF16), wide) == col_slot
    hi = spread.astype(BF16)
    lo = (spread - hi.astype(F32)).astype(BF16)
    sel_hi[...] = jnp.where(mine, nn_dot(hi, wide), 0.0).astype(BF16)
    sel_lo[...] = jnp.where(mine, nn_dot(lo, wide), 0.0).astype(BF16)

    def f1_copy(e, side):
        return rcopy(o1[side].at[e], o1[side].at[e], f1_s.at[e], f1_r.at[e], grp=mate)

    def f2_copy(j, side):
        part = o2.at[(eh // 2) * side + j]
        return rcopy(part, part, f2_s.at[j], f2_r.at[j], grp=mate)

    def fs_copy(side):
        return rcopy(osh.at[:, :, side], osh.at[:, :, side], fs_s, fs_r, grp=mate)

    def dd_copy(u):
        r0, n = unit_rows(u)
        rows = pl.ds(nx * r0, nx * n)
        return rcopy(pdo.at[rows], pdr.at[rows], dd_s.at[u], dd_r.at[u], tp=twin)

    def turn(k):
        return lax.rem(x + k * ahead + nx, nx)

    def rs_copy(u, arm, k):
        r0, n = unit_rows(u)
        rows = pl.ds(r0, n)
        goal, near, i = (turn(n_long - k), turn(1), k) if arm == 0 else (turn(k - n_short), turn(-1), n_long + k)
        return rcopy(q.at[goal, rows], rr.at[i, rows], rs_s.at[u, i], rs_r.at[u, i], tp=2 * near + core)

    def ag_copy(u, src, dst):
        r0, n = unit_rows(u)
        part = h.at[core, src, pl.ds(r0, n)]
        return rcopy(part, part, ag_s.at[u, dst], ag_r.at[u, src], tp=2 * dst + core)

    def fw_copy(u, src, side):
        r0, n = unit_rows(u)
        part = h.at[side, src, pl.ds(r0, n)]
        return rcopy(part, part, fw_s.at[u, src], fw_r.at[u, src], tp=twin)

    def re_copy(u, src, dst):
        rows = pl.ds(CAPACITY * u, CAPACITY)
        return rcopy(rb.at[dst, rows], rt.at[src, rows], re_s.at[u, dst], re_r.at[u, src], fs=dst)

    def paired(u, part):
        cols = pl.ds(pl.multiple_of(part * half, half), half)
        if u < eh:
            return jnp.concatenate([og[u, cols, :], ou[u, cols, :]], axis=0)
        zs = pl.ds(part * (nz // 2), nz // 2)
        return jnp.concatenate(
            [osh[0, zs].reshape(half, width), osh[1, zs].reshape(half, width)], axis=0
        )

    def first_matmul(u):
        r0, n = unit_rows(u)
        if u < eh:
            arrived = xr[...].astype(F32)[:, u * CAPACITY : (u + 1) * CAPACITY, :]
            rows_in = arrived.reshape(cap_rows, width).astype(BF16)
        else:
            rows_in = nrm_ref[...]
        pdo[nx * r0 : nx * (r0 + n), :] = nt_dot(rows_in, paired(u, 1 - core)).astype(BF16)
        dd_copy(u).start()
        own[nx * r0 : nx * (r0 + n), :] = nt_dot(rows_in, paired(u, core))

    def chip_sum(u):
        r0, n = unit_rows(u)
        rows = slice(nx * r0, nx * (r0 + n))
        dd_copy(u).wait_recv()
        both = own[rows, :] + pdr[rows, :].astype(F32)
        q[:, r0 : r0 + n, :] = both.astype(BF16).reshape(nx, n, 2 * half)
        rs_copy(u, 0, 0).start()
        rs_copy(u, 1, 0).start()

    def rs_step(u, k):
        r0, n = unit_rows(u)
        rows = slice(r0, r0 + n)
        for arm, steps in ((0, n_long), (1, n_short)):
            if k < steps:
                rs_copy(u, arm, k - 1).wait_recv()
                goal, i = (turn(n_long - k), k - 1) if arm == 0 else (turn(k - n_short), n_long + k - 1)
                q[goal, rows, :] = (q[goal, rows, :].astype(F32) + rr[i, rows, :].astype(F32)).astype(BF16)
                rs_copy(u, arm, k).start()

    def activate(u):
        r0, n = unit_rows(u)
        rows = slice(r0, r0 + n)
        rs_copy(u, 0, n_long - 1).wait_recv()
        rs_copy(u, 1, n_short - 1).wait_recv()
        pre = q[x, rows, :].astype(F32) + rr[n_long - 1, rows, :].astype(F32) + rr[nx - 2, rows, :].astype(F32)
        h[core, x, r0 : r0 + n, :] = (jax.nn.silu(pre[:, :half]) * pre[:, half:]).astype(BF16)
        each(nx, x, lambda d: ag_copy(u, x, d).start())
        fw_copy(u, x, core).start()

    def pass_on(u):
        def one(d):
            ag_copy(u, d, x).wait_recv()
            fw_copy(u, d, core).start()

        each(nx, x, one)

    def hidden_part(u, part):
        r0, n = unit_rows(u)
        return h[part, :, r0 : r0 + n, :].reshape(nx * n, half)

    def all_hidden(u):
        def one(k, carry):
            fw_copy(u, k, 1 - core).wait_recv()
            return carry

        lax.fori_loop(0, nx, one, 0)

    def arrivals(u):
        def one(side):
            each(nz, z, lambda d: w1_copy(side, u, d, z).wait_recv())
            f1_copy(u, side).start()

        if u < eh:
            on_side(one)
        else:
            each(nz, z, lambda d: sh_copy(d, z).wait_recv())
            fs_copy(y).start()

    def passed(u):
        if u < eh:
            on_side(lambda side: f1_copy(u, 1 - side).wait_recv())
        else:
            fs_copy(1 - y).wait_recv()

    order = tuple(range(units))
    arrivals(order[0])
    for i in range(units + 3):
        if i < units:
            passed(order[i])
            if i == 0:
                each(nz, z, lambda d: tk_copy(d, z).wait_recv())
            first_matmul(order[i])
        if 0 <= i - 1 < units:
            rs_step(order[i - 1], 1)
        if 0 <= i - 2 < units:
            rs_step(order[i - 2], 3)
        if i < units - 1:
            arrivals(order[i + 1])
        if i < units:
            chip_sum(order[i])
        if 0 <= i - 1 < units:
            rs_step(order[i - 1], 2)
        if 0 <= i - 2 < units:
            activate(order[i - 2])
        if 0 <= i - 3 < units:
            pass_on(order[i - 3])
        if i == units:
            for j in range(eh // 2):
                each(nz, z, lambda d: w2_copy(j, d, z).wait_recv())
                f2_copy(j, y).start()
            for store in stores[:2]:
                store.start()
            osg[...] = osh[0].reshape(ff, width)
            osu[...] = osh[1].reshape(ff, width)
            osd[...] = osh[2].reshape(ff, width)
            for store in stores[3:]:
                store.start()
        if i == units + 1:
            for j in range(eh // 2):
                f2_copy(j, 1 - y).wait_recv()
            for u in range(eh):
                all_hidden(u)
                res = nn_dot(hidden_part(u, 0), o2[u, :half, :]) + nn_dot(hidden_part(u, 1), o2[u, half:, :])
                rb[:, CAPACITY * u : CAPACITY * (u + 1), :] = res.reshape(nz, CAPACITY, width).astype(BF16)
                each(nz, z, lambda d: re_copy(u, z, d).start())
            stores[2].start()
    rt[z] = rb[z]
    all_hidden(eh)
    down = osh[2].reshape(ff, width)
    shared = nn_dot(hidden_part(eh, 0), down[:half]) + nn_dot(hidden_part(eh, 1), down[half:])
    for u in range(eh):
        each(nz, z, lambda d: re_copy(u, d, z).wait_recv())
    back = rt[...].reshape(experts * CAPACITY, width)
    out_ref[...] = (nn_dot(sel_hi[...], back) + nn_dot(sel_lo[...], back) + shared).astype(BF16)

    for store in stores:
        store.wait()
    each(nt, t, lambda d: stat_copy(t, d).wait_send())
    each(nz, z, lambda d: tk_copy(z, d).wait_send())

    def sent(side):
        for e in range(eh):
            each(nz, z, lambda d: w1_copy(side, e, z, d).wait_send())
            f1_copy(e, side).wait_send()

    on_side(sent)
    for j in range(eh // 2):
        each(nz, z, lambda d: w2_copy(j, z, d).wait_send())
        f2_copy(j, y).wait_send()
    each(nz, z, lambda d: sh_copy(z, d).wait_send())
    fs_copy(y).wait_send()
    for u in range(units):
        dd_copy(u).wait_send()
        for k in range(n_long):
            rs_copy(u, 0, k).wait_send()
        for k in range(n_short):
            rs_copy(u, 1, k).wait_send()
        each(nx, x, lambda d: ag_copy(u, x, d).wait_send())
        fw_copy(u, x, core).wait_send()
        each(nx, x, lambda d: fw_copy(u, d, core).wait_send())
    for u in range(eh):
        each(nz, z, lambda d: re_copy(u, z, d).wait_send())


def hand_over(*refs):
    n = len(refs) // 3
    took, gave = refs[3 * n], refs[3 * n + 1]
    ins = [pltpu.make_async_copy(refs[i], refs[2 * n + i], took.at[i]) for i in range(n)]
    outs = [pltpu.make_async_copy(refs[2 * n + i], refs[n + i], gave.at[i]) for i in range(n)]
    for copy in ins:
        copy.start()
    for i in range(n):
        ins[i].wait()
        outs[i].start()
    for copy in outs:
        copy.wait()


def on_device(nz, nt, tokens, norm_gain, expert_ids, route_scores, gate, up, down, sg, su, sd):
    experts, ff_here, width = gate.shape
    eh = experts // nz
    ff = ff_here * nz
    half = ff // 2
    toks = tokens.shape[0]
    nx = nt // 2
    rows = eh * nz * CAPACITY + toks
    disp = (nz, eh * CAPACITY, width)
    units = eh + 1
    vmem = pl.BlockSpec(memory_space=pltpu.VMEM)
    dma = pltpu.SemaphoreType.DMA
    pairs = eh // 2
    sems = []
    for shape in (
        (nt,), (nz,), (eh, nz), (eh,), (pairs, nz), (pairs,), (nz,), (), (units,), (units, nx - 1), (units, nx),
        (units, nx), (eh, nz),
    ):
        sems += [dma(shape), dma(shape)]
    anyw = pl.BlockSpec(memory_space=pl.ANY)
    made = pl.pallas_call(
        functools.partial(layer_kernel, nz, nt, width * nt),
        out_shape=(
            *([jax.ShapeDtypeStruct((eh, ff, width), BF16)] * 3),
            *([jax.ShapeDtypeStruct((ff, width), BF16)] * 3),
            jax.ShapeDtypeStruct((toks, width), BF16),
        ),
        in_specs=[vmem] * 4 + [anyw] * 3 + [vmem] * 3,
        out_specs=(anyw,) * 6 + (vmem,),
        scratch_shapes=[
            *([pltpu.VMEM((experts, ff_here, width), F32)] * 3),
            *([pltpu.VMEM((eh, ff, width), BF16)] * 3),
            *([pltpu.VMEM((ff, width), BF16)] * 3),
            dma((3,)),
            dma((6,)),
            pltpu.VMEM((3, nz, 2, ff_here // 2, width), BF16),
            pltpu.VMEM((2, experts, ff_here, width), BF16),
            pltpu.VMEM((experts, ff_here, width), BF16),
            pltpu.VMEM((3, 2, ff_here // 2, width), BF16),
            pltpu.VMEM((nt, 8, toks), F32),
            pltpu.VMEM(disp, BF16),
            pltpu.VMEM(disp, BF16),
            pltpu.VMEM((rows, 2 * half), F32),
            pltpu.VMEM((rows, 2 * half), BF16),
            pltpu.VMEM((rows, 2 * half), BF16),
            pltpu.VMEM((nx, rows // nx, 2 * half), BF16),
            pltpu.VMEM((nx - 1, rows // nx, 2 * half), BF16),
            pltpu.VMEM((2, nx, rows // nx, half), BF16),
            pltpu.VMEM(disp, BF16),
            pltpu.VMEM(disp, BF16),
            pltpu.VMEM((toks, experts * CAPACITY), BF16),
            pltpu.VMEM((toks, experts * CAPACITY), BF16),
            pltpu.VMEM((toks, width), BF16),
            *sems,
        ],
        compiler_params=pltpu.CompilerParams(
            collective_id=0, has_side_effects=True, vmem_limit_bytes=56 * 1024 * 1024
        ),
        name="layer",
    )(
        tokens, norm_gain.reshape(1, width), expert_ids.T, route_scores.T,
        gate, up, down, sg, su, sd,
    )
    return pl.pallas_call(
        hand_over,
        out_shape=tuple(jax.ShapeDtypeStruct(a.shape, a.dtype) for a in made),
        in_specs=[anyw] * len(made),
        out_specs=(anyw,) * len(made),
        scratch_shapes=[
            *(pltpu.VMEM(a.shape, a.dtype) for a in made),
            dma((len(made),)),
            dma((len(made),)),
        ],
        name="hand_over",
    )(*made)


def solution(mesh):
    return jax.shard_map(
        functools.partial(on_device, mesh.shape["fs"], mesh.shape["tp"]),
        mesh=mesh,
        in_specs=(
            P(("grp", "fs"), "tp"),
            P("tp"),
            P(("grp", "fs"), None),
            P(("grp", "fs"), None),
            P(None, "fs", "tp"),
            P(None, "fs", "tp"),
            P(None, "fs", "tp"),
            P("fs", "tp"),
            P("fs", "tp"),
            P("fs", "tp"),
        ),
        out_specs=(
            P(("grp", "fs"), None, "tp"),
            P(("grp", "fs"), None, "tp"),
            P(("grp", "fs"), None, "tp"),
            P("grp", "tp"),
            P("grp", "tp"),
            P("grp", "tp"),
            P(("grp", "fs"), "tp"),
        ),
        check_vma=False,
    )
```

```python
import functools

import jax
import jax.numpy as jnp
from jax import lax
from jax.experimental import pallas as pl
from jax.experimental.pallas import tpu as pltpu
from jax.sharding import PartitionSpec as P

CAPACITY = 24
NORM_EPS = 1e-05
ROUTED_SCALE = 2.5
MESH = pl.DeviceIdType.MESH
F32 = jnp.float32
BF16 = jnp.bfloat16


def nt_dot(a, b):
    return lax.dot_general(a, b, (((1,), (1,)), ((), ())), preferred_element_type=F32)


def nn_dot(a, b):
    return jnp.dot(a, b, preferred_element_type=F32)


def layer_kernel(
    nz, nt, full_width,
    tok_ref, gain_ref, ids_ref, score_ref, gate_hbm, up_hbm, down_hbm, sg_ref, su_ref, sd_ref,
    og_hbm, ou_hbm, od_hbm, osg_hbm, osu_hbm, osd_hbm, out_ref,
    gate_ref, up_ref, down_ref, og, ou, o2, osg, osu, osd, in_sem, out_sem,
    osh, w1, w2, ws, stat, xs, xr, own, pdo, pdr, q, rr, h, rb, rt, sel, nrm_ref,
    st_s, st_r, tk_s, tk_r, w1_s, w1_r, f1_s, f1_r, w2_s, w2_r, f2_s, f2_r, sh_s, sh_r, fs_s, fs_r,
    dd_s, dd_r, rs_s, rs_r, ag_s, ag_r, fw_s, fw_r, re_s, re_r,
):
    z = lax.axis_index("fs")
    t = lax.axis_index("tp")
    g = lax.axis_index("grp")
    y = lax.rem(g, 2)
    mate = g + 1 - 2 * y
    core = lax.rem(t, 2)
    x = t // 2
    nx = nt // 2
    twin = t + 1 - 2 * core
    ahead = 1 - 2 * core
    n_long = nx // 2
    n_short = nx - 1 - n_long
    o1 = (og, ou)

    experts, ff_here, width = gate_hbm.shape
    eh = experts // nz
    ff = ff_here * nz
    half = ff // 2
    toks = tok_ref.shape[0]
    cap_rows = nz * CAPACITY
    seg = cap_rows // nx
    sseg = toks // nx
    units = eh + 1

    def unit_rows(u):
        return (u * seg, seg) if u < eh else (eh * seg, sseg)

    def rcopy(src, dst, ss, rs, **where):
        return pltpu.make_async_remote_copy(
            src_ref=src, dst_ref=dst, send_sem=ss, recv_sem=rs, device_id=where, device_id_type=MESH
        )

    def each(n, me, body):
        def step(k, carry):
            body(lax.rem(me + k, n))
            return carry

        lax.fori_loop(1, n, step, 0)

    barrier = pltpu.get_barrier_semaphore()
    each(nz, z, lambda d: pl.semaphore_signal(barrier, inc=1, device_id={"fs": d}, device_id_type=MESH))
    each(nt, t, lambda d: pl.semaphore_signal(barrier, inc=1, device_id={"tp": d}, device_id_type=MESH))
    pl.semaphore_signal(barrier, inc=1, device_id={"grp": mate}, device_id_type=MESH)

    loads = [
        pltpu.make_async_copy(src, dst, in_sem.at[i])
        for i, (src, dst) in enumerate(((gate_hbm, gate_ref), (up_hbm, up_ref), (down_hbm, down_ref)))
    ]
    for load in loads:
        load.start()
    stores = [
        pltpu.make_async_copy(src, dst, out_sem.at[i])
        for i, (src, dst) in enumerate(
            ((og, og_hbm), (ou, ou_hbm), (o2, od_hbm), (osg, osg_hbm), (osu, osu_hbm), (osd, osd_hbm))
        )
    ]
    gain = gain_ref[...]
    hr = ff_here // 2
    ws[0] = (sg_ref[...] * gain).astype(BF16).reshape(2, hr, width)
    ws[1] = (su_ref[...] * gain).astype(BF16).reshape(2, hr, width)
    ws[2] = sd_ref[...].astype(BF16).reshape(2, hr, width)
    loads[0].wait()
    w1[0] = (gate_ref[...] * gain[None]).astype(BF16)
    loads[1].wait()
    w1[1] = (up_ref[...] * gain[None]).astype(BF16)
    loads[2].wait()
    w2[...] = down_ref[...].astype(BF16)
    rows_z = pl.ds(pl.multiple_of(z * ff_here, ff_here), ff_here)

    def on_side(body):
        for side in (0, 1):
            pl.when(y == side)(functools.partial(body, side))

    def keep_own(side):
        o1[side][:, rows_z, :] = w1[side, pl.ds(eh * z, eh)]

    on_side(keep_own)
    o2[pl.ds((eh // 2) * y, eh // 2), rows_z, :] = w2[pl.ds(eh * z + (eh // 2) * y, eh // 2)]
    osh[:, z, y] = ws[:, y]

    tok_t = tok_ref[...].astype(F32).T
    stat[t] = jnp.concatenate(
        [
            jnp.sum(tok_t, axis=0, keepdims=True),
            jnp.sum(tok_t * tok_t, axis=0, keepdims=True),
            jnp.zeros((6, toks), F32),
        ],
        axis=0,
    )

    pl.semaphore_wait(barrier, nz + nt - 1)

    def stat_copy(src, dst):
        return rcopy(stat.at[src], stat.at[src], st_s.at[dst], st_r.at[src], tp=dst)

    each(nt, t, lambda d: stat_copy(t, d).start())

    def w1_copy(side, e, src, dst):
        return rcopy(
            w1.at[side, eh * dst + e],
            o1[side].at[e, pl.ds(pl.multiple_of(src * ff_here, ff_here), ff_here), :],
            w1_s.at[e, dst], w1_r.at[e, src], fs=dst,
        )

    def w2_copy(j, src, dst):
        return rcopy(
            w2.at[eh * dst + (eh // 2) * y + j],
            o2.at[(eh // 2) * y + j, pl.ds(pl.multiple_of(src * ff_here, ff_here), ff_here), :],
            w2_s.at[j, dst], w2_r.at[j, src], fs=dst,
        )

    def sh_copy(src, dst):
        return rcopy(ws.at[:, y], osh.at[:, src, y], sh_s.at[dst], sh_r.at[src], fs=dst)

    def tk_copy(u, src, dst):
        rows = pl.ds(CAPACITY * u, CAPACITY)
        return rcopy(xs.at[dst, rows], xr.at[src, rows], tk_s.at[u, dst], tk_r.at[u, src], fs=dst)

    def send_w1(first, last):
        def one(side):
            for e in range(first, last):
                each(nz, z, lambda d: w1_copy(side, e, z, d).start())

        on_side(one)

    send_w1(0, 1)

    ids = ids_ref[...]
    scores = score_ref[...]
    weight = scores / jnp.sum(scores, axis=0, keepdims=True) * ROUTED_SCALE
    expert = lax.broadcasted_iota(jnp.int32, (experts, toks), 0)
    chosen = jnp.zeros((experts, toks), F32)
    spread = jnp.zeros((experts, toks), F32)
    for k in range(ids.shape[0]):
        hit = ids[k : k + 1] == expert
        chosen = chosen + jnp.where(hit, 1.0, 0.0)
        spread = spread + jnp.where(hit, weight[k : k + 1], 0.0)
    above = lax.broadcasted_iota(jnp.int32, (toks, toks), 0) < lax.broadcasted_iota(
        jnp.int32, (toks, toks), 1
    )
    rank_t = nn_dot(chosen.astype(BF16), jnp.where(above, 1.0, 0.0).astype(BF16))
    rank_t = jnp.where(chosen > 0.5, rank_t, -1.0)
    slot = lax.broadcasted_iota(jnp.int32, (experts, CAPACITY, toks), 1).astype(F32)
    pick = jnp.where(rank_t[:, None, :] == slot, 1.0, 0.0).reshape(experts * CAPACITY, toks)
    pick = pick.astype(BF16)

    each(nt, t, lambda d: stat_copy(d, t).wait_recv())
    total = jnp.sum(stat[...], axis=0)
    mean = total[0:1] / full_width
    var = total[1:2] / full_width - mean * mean
    nrm = ((tok_t - mean) * lax.rsqrt(var + NORM_EPS)).T.astype(BF16)
    nrm_ref[...] = nrm
    xs[...] = nn_dot(pick, nrm).astype(BF16).reshape(nz, eh * CAPACITY, width)
    for u in range(eh):
        each(nz, z, lambda d: tk_copy(u, z, d).start())
        if u + 1 < eh:
            send_w1(u + 1, u + 2)
    for j in range(eh // 2):
        each(nz, z, lambda d: w2_copy(j, z, d).start())
    each(nz, z, lambda d: sh_copy(z, d).start())

    xr[z] = xs[z]
    rank = jnp.concatenate([rank_t, jnp.full((toks - experts, toks), -1.0, F32)], axis=0).T
    spread = jnp.concatenate([spread, jnp.zeros((toks - experts, toks), F32)], axis=0).T
    row = lax.broadcasted_iota(jnp.int32, (toks, experts * CAPACITY), 0) * CAPACITY
    col = lax.broadcasted_iota(jnp.int32, (toks, experts * CAPACITY), 1)
    wide = jnp.where((col >= row) & (col < row + CAPACITY), 1.0, 0.0).astype(BF16)
    colf = col.astype(F32)
    col_slot = colf - jnp.floor((colf + 0.5) * (1.0 / CAPACITY)) * CAPACITY
    mine = nn_dot(rank.astype(BF16), wide) == col_slot
    hi = spread.astype(BF16)
    lo = (spread - hi.astype(F32)).astype(BF16)
    sel[:toks, :] = jnp.where(mine, nn_dot(hi, wide), 0.0).astype(BF16)
    sel[toks:, :] = jnp.where(mine, nn_dot(lo, wide), 0.0).astype(BF16)

    def f1_copy(e, side):
        return rcopy(o1[side].at[e], o1[side].at[e], f1_s.at[e], f1_r.at[e], grp=mate)

    def f2_copy(j, side):
        part = o2.at[(eh // 2) * side + j]
        return rcopy(part, part, f2_s.at[j], f2_r.at[j], grp=mate)

    def fs_copy(side):
        return rcopy(osh.at[:, :, side], osh.at[:, :, side], fs_s, fs_r, grp=mate)

    def dd_copy(u):
        r0, n = unit_rows(u)
        rows = pl.ds(nx * r0, nx * n)
        return rcopy(pdo.at[rows], pdr.at[rows], dd_s.at[u], dd_r.at[u], tp=twin)

    def turn(k):
        return lax.rem(x + k * ahead + nx, nx)

    def across(k):
        rows = pl.ds(*unit_rows(eh))
        goal = lax.rem(x + k, nx)
        return rcopy(
            q.at[goal, rows], rr.at[k - 1, rows], rs_s.at[eh, k - 1], rs_r.at[eh, k - 1], tp=2 * goal + core
        )

    def rs_copy(u, arm, k):
        r0, n = unit_rows(u)
        rows = pl.ds(r0, n)
        goal, near, i = (turn(n_long - k), turn(1), k) if arm == 0 else (turn(k - n_short), turn(-1), n_long + k)
        return rcopy(q.at[goal, rows], rr.at[i, rows], rs_s.at[u, i], rs_r.at[u, i], tp=2 * near + core)

    def ag_copy(u, src, dst):
        r0, n = unit_rows(u)
        part = h.at[core, src, pl.ds(r0, n)]
        return rcopy(part, part, ag_s.at[u, dst], ag_r.at[u, src], tp=2 * dst + core)

    def fw_copy(u, src, side):
        r0, n = unit_rows(u)
        part = h.at[side, src, pl.ds(r0, n)]
        return rcopy(part, part, fw_s.at[u, src], fw_r.at[u, src], tp=twin)

    def re_copy(u, src, dst):
        rows = pl.ds(CAPACITY * u, CAPACITY)
        return rcopy(rb.at[dst, rows], rt.at[src, rows], re_s.at[u, dst], re_r.at[u, src], fs=dst)

    def paired(u, part):
        cols = pl.ds(pl.multiple_of(part * half, half), half)
        if u < eh:
            return jnp.concatenate([og[u, cols, :], ou[u, cols, :]], axis=0)
        zs = pl.ds(part * (nz // 2), nz // 2)
        return jnp.concatenate(
            [osh[0, zs].reshape(half, width), osh[1, zs].reshape(half, width)], axis=0
        )

    def first_matmul(u):
        r0, n = unit_rows(u)
        if u < eh:
            arrived = xr[:, u * CAPACITY : (u + 1) * CAPACITY, :].astype(F32)
            rows_in = arrived.reshape(cap_rows, width).astype(BF16)
        else:
            rows_in = nrm_ref[...]
        pdo[nx * r0 : nx * (r0 + n), :] = nt_dot(rows_in, paired(u, 1 - core)).astype(BF16)
        dd_copy(u).start()
        own[nx * r0 : nx * (r0 + n), :] = nt_dot(rows_in, paired(u, core))

    def chip_sum(u):
        r0, n = unit_rows(u)
        rows = slice(nx * r0, nx * (r0 + n))
        dd_copy(u).wait_recv()
        both = own[rows, :] + pdr[rows, :].astype(F32)
        q[:, r0 : r0 + n, :] = both.astype(BF16).reshape(nx, n, 2 * half)
        if u == eh:
            for k in range(1, nx):
                across(k).start()
        else:
            rs_copy(u, 0, 0).start()
            rs_copy(u, 1, 0).start()

    def rs_step(u, k):
        r0, n = unit_rows(u)
        rows = slice(r0, r0 + n)
        for arm, steps in ((0, n_long), (1, n_short)):
            if k < steps:
                rs_copy(u, arm, k - 1).wait_recv()
                goal, i = (turn(n_long - k), k - 1) if arm == 0 else (turn(k - n_short), n_long + k - 1)
                q[goal, rows, :] = (q[goal, rows, :].astype(F32) + rr[i, rows, :].astype(F32)).astype(BF16)
                rs_copy(u, arm, k).start()

    def activate(u):
        r0, n = unit_rows(u)
        rows = slice(r0, r0 + n)
        pre = q[x, rows, :].astype(F32)
        if u == eh:
            for k in range(1, nx):
                across(k).wait_recv()
            pre = pre + jnp.sum(rr[:, rows, :].astype(F32), axis=0)
        else:
            rs_copy(u, 0, n_long - 1).wait_recv()
            rs_copy(u, 1, n_short - 1).wait_recv()
            pre = pre + rr[n_long - 1, rows, :].astype(F32) + rr[nx - 2, rows, :].astype(F32)
        h[core, x, r0 : r0 + n, :] = (jax.nn.silu(pre[:, :half]) * pre[:, half:]).astype(BF16)
        each(nx, x, lambda d: ag_copy(u, x, d).start())
        fw_copy(u, x, core).start()

    def pass_on(u):
        def one(d):
            ag_copy(u, d, x).wait_recv()
            fw_copy(u, d, core).start()

        each(nx, x, one)

    def hidden_part(u, part):
        r0, n = unit_rows(u)
        return h[part, :, r0 : r0 + n, :].reshape(nx * n, half)

    def all_hidden(u):
        def one(k, carry):
            fw_copy(u, k, 1 - core).wait_recv()
            return carry

        lax.fori_loop(0, nx, one, 0)

    def arrivals(u):
        def one(side):
            each(nz, z, lambda d: w1_copy(side, u, d, z).wait_recv())
            f1_copy(u, side).start()

        if u < eh:
            on_side(one)
        else:
            each(nz, z, lambda d: sh_copy(d, z).wait_recv())
            fs_copy(y).start()

    def passed(u):
        if u < eh:
            on_side(lambda side: f1_copy(u, 1 - side).wait_recv())
        else:
            fs_copy(1 - y).wait_recv()

    def second_matmul(u):
        all_hidden(u)
        res = nn_dot(hidden_part(u, 0), o2[u, :half, :]) + nn_dot(hidden_part(u, 1), o2[u, half:, :])
        rb[:, CAPACITY * u : CAPACITY * (u + 1), :] = res.reshape(nz, CAPACITY, width).astype(BF16)
        each(nz, z, lambda d: re_copy(u, z, d).start())

    arrivals(0)
    for i in range(eh + 2):
        if i < eh:
            passed(i)
            each(nz, z, lambda d: tk_copy(i, d, z).wait_recv())
            first_matmul(i)
        if 0 <= i - 1 < eh:
            rs_step(i - 1, 1)
        if 0 <= i - 2 < eh:
            rs_step(i - 2, 3)
        if i < eh - 1:
            arrivals(i + 1)
        if i < eh:
            chip_sum(i)
        if 0 <= i - 1 < eh:
            rs_step(i - 1, 2)
        if 0 <= i - 2 < eh:
            activate(i - 2)
        if 0 <= i - 3 < eh:
            pass_on(i - 3)
        if i == eh:
            for j in range(eh // 2):
                each(nz, z, lambda d: w2_copy(j, d, z).wait_recv())
                f2_copy(j, y).start()
            for store in stores[:2]:
                store.start()
    for j in range(eh // 2):
        f2_copy(j, 1 - y).wait_recv()
    for u in range(eh - 1):
        second_matmul(u)
    arrivals(eh)
    pass_on(eh - 1)
    second_matmul(eh - 1)
    passed(eh)
    first_matmul(eh)
    chip_sum(eh)
    stores[2].start()
    osg[...] = osh[0].reshape(ff, width)
    osu[...] = osh[1].reshape(ff, width)
    osd[...] = osh[2].reshape(ff, width)
    for store in stores[3:]:
        store.start()
    activate(eh)
    pass_on(eh)
    rt[z] = rb[z]
    all_hidden(eh)
    down = osh[2].reshape(ff, width)
    shared = nn_dot(hidden_part(eh, 0), down[:half]) + nn_dot(hidden_part(eh, 1), down[half:])
    for store in stores:
        store.wait()
    each(nt, t, lambda d: stat_copy(t, d).wait_send())
    for u in range(eh):
        each(nz, z, lambda d: tk_copy(u, z, d).wait_send())

    def sent(side):
        for e in range(eh):
            each(nz, z, lambda d: w1_copy(side, e, z, d).wait_send())
            f1_copy(e, side).wait_send()

    on_side(sent)
    for j in range(eh // 2):
        each(nz, z, lambda d: w2_copy(j, z, d).wait_send())
        f2_copy(j, y).wait_send()
    each(nz, z, lambda d: sh_copy(z, d).wait_send())
    fs_copy(y).wait_send()
    for u in range(units):
        dd_copy(u).wait_send()
        if u == eh:
            for k in range(1, nx):
                across(k).wait_send()
        else:
            for k in range(n_long):
                rs_copy(u, 0, k).wait_send()
            for k in range(n_short):
                rs_copy(u, 1, k).wait_send()
        each(nx, x, lambda d: ag_copy(u, x, d).wait_send())
        fw_copy(u, x, core).wait_send()
        each(nx, x, lambda d: fw_copy(u, d, core).wait_send())
    for u in range(eh):
        each(nz, z, lambda d: re_copy(u, z, d).wait_send())
    for u in range(eh):
        each(nz, z, lambda d: re_copy(u, d, z).wait_recv())
    back = rt[...].reshape(experts * CAPACITY, width)
    mixed = nn_dot(sel[...], back)
    out_ref[...] = (mixed[:toks] + mixed[toks:] + shared).astype(BF16)


def hand_over(*refs):
    n = len(refs) // 3
    took, gave = refs[3 * n], refs[3 * n + 1]
    ins = [pltpu.make_async_copy(refs[i], refs[2 * n + i], took.at[i]) for i in range(n)]
    outs = [pltpu.make_async_copy(refs[2 * n + i], refs[n + i], gave.at[i]) for i in range(n)]
    for copy in ins:
        copy.start()
    for i in range(n):
        ins[i].wait()
        outs[i].start()
    for copy in outs:
        copy.wait()


def on_device(nz, nt, tokens, norm_gain, expert_ids, route_scores, gate, up, down, sg, su, sd):
    experts, ff_here, width = gate.shape
    eh = experts // nz
    ff = ff_here * nz
    half = ff // 2
    toks = tokens.shape[0]
    nx = nt // 2
    rows = eh * nz * CAPACITY + toks
    disp = (nz, eh * CAPACITY, width)
    units = eh + 1
    vmem = pl.BlockSpec(memory_space=pltpu.VMEM)
    dma = pltpu.SemaphoreType.DMA
    pairs = eh // 2
    sems = []
    for shape in (
        (nt,), (eh, nz), (eh, nz), (eh,), (pairs, nz), (pairs,), (nz,), (), (units,), (units, nx - 1), (units, nx),
        (units, nx), (eh, nz),
    ):
        sems += [dma(shape), dma(shape)]
    anyw = pl.BlockSpec(memory_space=pl.ANY)
    made = pl.pallas_call(
        functools.partial(layer_kernel, nz, nt, width * nt),
        out_shape=(
            *([jax.ShapeDtypeStruct((eh, ff, width), BF16)] * 3),
            *([jax.ShapeDtypeStruct((ff, width), BF16)] * 3),
            jax.ShapeDtypeStruct((toks, width), BF16),
        ),
        in_specs=[vmem] * 4 + [anyw] * 3 + [vmem] * 3,
        out_specs=(anyw,) * 6 + (vmem,),
        scratch_shapes=[
            *([pltpu.VMEM((experts, ff_here, width), F32)] * 3),
            *([pltpu.VMEM((eh, ff, width), BF16)] * 3),
            *([pltpu.VMEM((ff, width), BF16)] * 3),
            dma((3,)),
            dma((6,)),
            pltpu.VMEM((3, nz, 2, ff_here // 2, width), BF16),
            pltpu.VMEM((2, experts, ff_here, width), BF16),
            pltpu.VMEM((experts, ff_here, width), BF16),
            pltpu.VMEM((3, 2, ff_here // 2, width), BF16),
            pltpu.VMEM((nt, 8, toks), F32),
            pltpu.VMEM(disp, BF16),
            pltpu.VMEM(disp, BF16),
            pltpu.VMEM((rows, 2 * half), F32),
            pltpu.VMEM((rows, 2 * half), BF16),
            pltpu.VMEM((rows, 2 * half), BF16),
            pltpu.VMEM((nx, rows // nx, 2 * half), BF16),
            pltpu.VMEM((nx - 1, rows // nx, 2 * half), BF16),
            pltpu.VMEM((2, nx, rows // nx, half), BF16),
            pltpu.VMEM(disp, BF16),
            pltpu.VMEM(disp, BF16),
            pltpu.VMEM((2 * toks, experts * CAPACITY), BF16),
            pltpu.VMEM((toks, width), BF16),
            *sems,
        ],
        compiler_params=pltpu.CompilerParams(
            collective_id=0, has_side_effects=True, vmem_limit_bytes=56 * 1024 * 1024
        ),
        name="layer",
    )(
        tokens, norm_gain.reshape(1, width), expert_ids.T, route_scores.T,
        gate, up, down, sg, su, sd,
    )
    return pl.pallas_call(
        hand_over,
        out_shape=tuple(jax.ShapeDtypeStruct(a.shape, a.dtype) for a in made),
        in_specs=[anyw] * len(made),
        out_specs=(anyw,) * len(made),
        scratch_shapes=[
            *(pltpu.VMEM(a.shape, a.dtype) for a in made),
            dma((len(made),)),
            dma((len(made),)),
        ],
        name="hand_over",
    )(*made)


def solution(mesh):
    return jax.shard_map(
        functools.partial(on_device, mesh.shape["fs"], mesh.shape["tp"]),
        mesh=mesh,
        in_specs=(
            P(("grp", "fs"), "tp"),
            P("tp"),
            P(("grp", "fs"), None),
            P(("grp", "fs"), None),
            P(None, "fs", "tp"),
            P(None, "fs", "tp"),
            P(None, "fs", "tp"),
            P("fs", "tp"),
            P("fs", "tp"),
            P("fs", "tp"),
        ),
        out_specs=(
            P(("grp", "fs"), None, "tp"),
            P(("grp", "fs"), None, "tp"),
            P(("grp", "fs"), None, "tp"),
            P("grp", "tp"),
            P("grp", "tp"),
            P("grp", "tp"),
            P(("grp", "fs"), "tp"),
        ),
        check_vma=False,
    )
```
